32 devices in a mesh: ep: 8 (over z, x), tp: 4 (over y, core).
Axes of the slice: x: 2, y: 2, z: 4, core: 2. Of those that a mesh axis runs over, the one named last changes fastest.
Arguments:
- tokens: bfloat16 [128, 2048], P('ep'), may hold values from -6 to 6
- attn_gain: float32 [2048], replicated, may hold values from 0.1 to 1.9
- w_query: bfloat16 [2048, 1024], P(None, 'tp'), may hold values from -0.125 to 0.125
- stick_bias: float32 [16], P('tp'), may hold values from -8.5 to -2.5
- kv_cache: bfloat16 [128, 8, 1024, 128], P('ep', 'tp'), may hold values from -6 to 6
- lengths: int32 [128], P('ep'), may hold values from 1 to 1024, as said below
- head_gain: float32 [1024], P('tp'), may hold values from 0.1 to 1.9
- w_attn_out: bfloat16 [1024, 2048], P('tp'), may hold values from -0.1875 to 0.1875
- ffn_gain: float32 [2048], replicated, may hold values from 0.1 to 1.9
- route_expert: int32 [128, 2], P('ep'), may hold values from 0 to 31, as said below
- route_weight: bfloat16 [128, 2], P('ep'), may hold values from 0.049804688 to 1
- w_exp_gate: bfloat16 [32, 2048, 2048], P('ep', None, 'tp'), may hold values from -0.125 to 0.125
- w_exp_up: bfloat16 [32, 2048, 2048], P('ep', None, 'tp'), may hold values from -0.125 to 0.125
- w_exp_down: bfloat16 [32, 2048, 2048], P('ep', 'tp'), may hold values from -0.125 to 0.125
- branch_gate: bfloat16 [2048], replicated, may hold values from -0.125 to 0.125
- w_dense_gate: bfloat16 [8192, 2048], P(('ep', 'tp')), may hold values from -0.125 to 0.125
- w_dense_up: bfloat16 [8192, 2048], P(('ep', 'tp')), may hold values from -0.125 to 0.125
- w_dense_down: bfloat16 [8192, 2048], P(('ep', 'tp')), may hold values from -0.125 to 0.125
Outputs:
- mixed: bfloat16 [128, 2048], P('ep', 'tp')
The draws below stay inside these ranges and needn't reach their ends.
Inputs may be any that keep to these rules, and one draw needn't show every extreme that they name: `route_expert`: each row names 2 different experts of one group (expert x lies in group x // 8). The rows of one index of ep name no expert more than 2 times; one group, the same for every index of ep, has each of its experts named exactly 2 times by the rows of every index of ep. `lengths`: some sequence has length 1024.
All inputs are finite; a program needn't handle non-finite values.
Results may differ from the reference program's by a relative error of at most 0.0076.
Values may be sent and summed in bfloat16 or wider, within the bound.
A program may use at most 128 MiB of HBM per device.

```python
import math
import jax
import jax.numpy as jnp
from jax import lax

D = 2048
HEADS = 16
HEAD = 64
KV_HEADS = 8
CACHE = 1024
SEQ_DEV = 16
GROUPS = 4
EPG = 8
TOPK = 2
EXP_FF = 2048
DENSE_FF = 8192
EXPERTS = 32
CAP = 2
SEQS = 128
N_EP = 8


def draw_stick_bias(key, part):
    return jax.random.uniform(key, (HEADS,), jnp.float32, -8.0, -2.5)


def draw_lengths(key, part):
    base_key = jax.random.fold_in(key, 5)
    key_shift, key_length, key_row = jax.random.split(base_key, 3)
    block_count = SEQS // SEQ_DEV
    shift_exp = jax.random.randint(key_shift, (block_count, 1), 0, 4)
    block_top = CACHE // jnp.power(2, shift_exp)
    drawn = jax.random.randint(key_length, (block_count, SEQ_DEV), 1, block_top + 1).reshape(SEQS)
    full_row = jax.random.randint(key_row, (), 0, SEQS)
    return jnp.where(jnp.arange(SEQS) == full_row, CACHE, drawn).astype(jnp.int32)


def draw_route_expert(key, part):
    base_key = jax.random.fold_in(key, 11)
    key_group, key_blocks = jax.random.split(base_key)
    most_rows = EPG * CAP // TOPK
    spare_slots = (GROUPS - 1) * most_rows
    full_group = jax.random.randint(key_group, (), 0, GROUPS)
    block_keys = jax.random.split(key_blocks, SEQS // SEQ_DEV)

    def one_block(block_key):
        key_order, key_slots, key_inner = jax.random.split(block_key, 3)
        order = jax.random.permutation(key_order, SEQ_DEV)
        slots = jax.random.permutation(key_slots, spare_slots)
        place = jnp.arange(SEQ_DEV)
        spare = jnp.take(slots, jnp.clip(place - most_rows, 0, spare_slots - 1))
        group_at = jnp.where(place < most_rows, full_group, (full_group + 1 + spare // most_rows) % GROUPS)
        group_of = jnp.zeros((SEQ_DEV,), jnp.int32).at[order].set(group_at.astype(jnp.int32))
        member = (group_of[:, None] == jnp.arange(GROUPS)[None, :]).astype(jnp.int32)
        slot_rank = jnp.sum(member * (jnp.cumsum(member, axis=0) - 1), axis=1)
        inner_scores = jax.random.randint(key_inner, (GROUPS, EPG), 0, 1 << 20) * EPG + jnp.arange(EPG)[None, :]
        inner_order = jnp.argsort(inner_scores, axis=1)
        pick = (TOPK * slot_rank[:, None] + jnp.arange(TOPK)[None, :]) % EPG
        inner = inner_order[group_of[:, None], pick]
        return group_of[:, None] * EPG + inner
    routes = jax.vmap(one_block)(block_keys)
    return routes.reshape(SEQS, TOPK).astype(jnp.int32)


def raised(values, rng, source, target, parts, factor):
    def block_of(axis_at):
        return (jnp.arange(values.shape[axis_at]) // (values.shape[axis_at] // parts)).reshape((-1,) + (1,) * (values.ndim - 1 - axis_at))

    one_side = jax.random.permutation(rng, parts)[block_of(target)]
    other_side = (block_of(target) + parts // 2) % parts
    return jnp.where((block_of(source) == one_side) | (block_of(source) == other_side), factor * values, values)


def block_scale(own_key, extent, pieces, least, top_value):
    level, own = 1.0, jax.random.fold_in(own_key, 6)
    for dim, shards_of in pieces:
        draws = jnp.exp(jax.random.uniform(jax.random.fold_in(own, dim), (shards_of,), jnp.float32, least / len(pieces), top_value / len(pieces)))
        level = level * jnp.repeat(draws, extent[dim] // shards_of).reshape([-1 if axis == dim else 1 for axis in range(len(extent))])
    return level


def scatter_about(stream_key, extent, scale, bound, cuts=(), kind=jnp.bfloat16):
    factor_of = block_scale(stream_key, extent, cuts, -0.22, 0.18) if cuts else 1.0
    values = jax.random.normal(stream_key, extent, jnp.float32) * scale * factor_of
    return jnp.minimum(jnp.maximum(values, -bound), bound).astype(kind)


def bell_draw_with(own_key, shape, scale, limit, pieces, heavy, kind=jnp.bfloat16):
    values = scale * jax.random.normal(own_key, shape, jnp.float32)
    if pieces:
        values = values * block_scale(own_key, shape, pieces, -0.22, 0.18)
    return jnp.clip(raised(values, jax.random.fold_in(own_key, 3), *heavy), -limit, limit).astype(kind)


def setup_inputs(seed: int = 0) -> dict:
    key_of = jax.random.split(jax.random.key(seed), 19)
    return {
        "tokens": scatter_about(key_of[0], (SEQS, D), 1.0, 6.0, ((0, 8),)),
        "attn_gain": jnp.clip(1.0 + 0.18 * jax.random.normal(key_of[1], (D,), jnp.float32), 0.1, 1.9),
        "w_query": scatter_about(key_of[2], (D, HEADS * HEAD), D ** -0.5, 0.125, ((1, 4),)),
        "stick_bias": draw_stick_bias(jax.random.fold_in(key_of[18], 71), 0),
        "kv_cache": scatter_about(key_of[4], (SEQS, KV_HEADS, CACHE, 2 * HEAD), 1.0, 6.0, ((0, 8), (1, 4))),
        "lengths": draw_lengths(jax.random.fold_in(key_of[18], 71), 0),
        "head_gain": jnp.clip(1.0 + 0.18 * jax.random.normal(key_of[6], (HEADS * HEAD,), jnp.float32), 0.1, 1.9),
        "w_attn_out": scatter_about(key_of[7], (HEADS * HEAD, D), (HEADS * HEAD) ** -0.5, 0.1875, ((0, 4),)),
        "ffn_gain": jnp.clip(1.0 + 0.18 * jax.random.normal(key_of[8], (D,), jnp.float32), 0.1, 1.9),
        "route_expert": draw_route_expert(jax.random.fold_in(key_of[18], 71), 0),
        "route_weight": jnp.clip(jnp.exp(math.log(1.0) - 2.9996462 * jax.random.uniform(key_of[10], (SEQS, TOPK), jnp.float32) ** block_scale(key_of[10], (SEQS, TOPK), ((0, 8),), -0.2, 0.2)), 0.049804688, 1.0).astype(jnp.bfloat16),
        "w_exp_gate": scatter_about(key_of[11], (EXPERTS, D, EXP_FF), D ** -0.5, 0.125, ((0, 8), (2, 4))),
        "w_exp_up": scatter_about(key_of[12], (EXPERTS, D, EXP_FF), D ** -0.5, 0.125, ((0, 8), (2, 4))),
        "w_exp_down": scatter_about(key_of[13], (EXPERTS, EXP_FF, D), EXP_FF ** -0.5, 0.125, ((0, 8), (1, 4))),
        "branch_gate": scatter_about(key_of[14], (D,), D ** -0.5, 0.125),
        "w_dense_gate": scatter_about(key_of[15], (DENSE_FF, D), D ** -0.5, 0.125, ((0, 32),)),
        "w_dense_up": scatter_about(key_of[16], (DENSE_FF, D), D ** -0.5, 0.125, ((0, 32),)),
        "w_dense_down": bell_draw_with(key_of[17], (DENSE_FF, D), DENSE_FF ** -0.5, 0.125, ((0, 32),), (0, 1, 32, 2.75)),
    }


epsilon = 1e-06
highest = lax.Precision.HIGHEST

def stored(values):
    return lax.optimization_barrier(values.astype(jnp.bfloat16))

def rms_scale(matrix, gain):
    wide = matrix.astype(jnp.float32)
    return wide * lax.rsqrt(lax.optimization_barrier(jnp.mean(wide * wide, axis=-1, keepdims=True)) + epsilon) * gain

def reference(tokens, attn_gain, w_query, stick_bias, kv_cache, lengths, head_gain, w_attn_out, ffn_gain, route_expert, route_weight, w_exp_gate, w_exp_up, w_exp_down, branch_gate, w_dense_gate, w_dense_up, w_dense_down):
    single = jnp.float32
    group_size = HEADS // KV_HEADS
    normed = stored(rms_scale(tokens, attn_gain))
    query_rows = stored(jnp.dot(normed, w_query, preferred_element_type=single))
    query_rows = query_rows.reshape(N_EP, SEQ_DEV, KV_HEADS, group_size, HEAD)
    cache_blocks = kv_cache.reshape(N_EP, SEQ_DEV, KV_HEADS, CACHE, 2 * HEAD)
    length_blocks = lengths.reshape(N_EP, SEQ_DEV)
    bias_grid = stick_bias.reshape(KV_HEADS, group_size)
    gain_grid = head_gain.reshape(KV_HEADS, group_size, HEAD)

    def attend(item_block):
        query_block, cache_block, length_block = item_block
        key_cols = cache_block[..., :HEAD].astype(single)
        value_cols = cache_block[..., HEAD:].astype(single)
        scores = jnp.einsum('shge,shke->shgk', query_block.astype(single), key_cols, precision=highest)
        scores = scores / math.sqrt(HEAD) + bias_grid[None, :, :, None]
        position = lax.broadcasted_iota(jnp.int32, scores.shape, 3)
        valid_keys = position < length_block[:, None, None, None]
        log_keep = jnp.where(valid_keys, -jax.nn.softplus(scores), 0.0)
        later_sum = lax.cumsum(log_keep, axis=3, reverse=True) - log_keep
        weights = jnp.where(valid_keys, jnp.exp(jax.nn.log_sigmoid(scores) + later_sum), 0.0)
        weights = stored(weights).astype(single)
        head_out = jnp.einsum('shgk,shke->shge', weights, value_cols, precision=highest)
        head_out = head_out * lax.rsqrt(lax.optimization_barrier(jnp.mean(head_out * head_out, axis=-1, keepdims=True)) + epsilon) * gain_grid
        return stored(head_out).reshape(SEQ_DEV, HEADS * HEAD)
    head_rows = lax.map(attend, (query_rows, cache_blocks, length_blocks)).reshape(SEQS, HEADS * HEAD)
    residual = tokens.astype(single) + jnp.dot(head_rows, w_attn_out, preferred_element_type=single)
    normed2 = stored(rms_scale(residual, ffn_gain))
    branch_weight = stored(jax.nn.sigmoid(jnp.dot(normed2, branch_gate, preferred_element_type=single)))
    branch_weight = branch_weight.astype(single)

    def expert_step(running, expert_index):
        hit_table = route_expert == expert_index
        row_weight = lax.optimization_barrier(jnp.sum(jnp.where(hit_table, route_weight.astype(single), 0.0), axis=1))
        used_rows = jnp.any(hit_table, axis=1)
        picked = jnp.nonzero(used_rows, size=N_EP * CAP, fill_value=0)[0].astype(jnp.int32)
        live_rows = jnp.arange(N_EP * CAP, dtype=jnp.int32) < jnp.sum(used_rows.astype(jnp.int32))
        chosen = jnp.take(normed2, picked, axis=0)
        gate_pre = jnp.dot(chosen, lax.dynamic_index_in_dim(w_exp_gate, expert_index, 0, False), preferred_element_type=single)
        up_pre = jnp.dot(chosen, lax.dynamic_index_in_dim(w_exp_up, expert_index, 0, False), preferred_element_type=single)
        hidden = (jax.nn.silu(gate_pre) * up_pre).astype(jnp.bfloat16)
        expert_out = jnp.dot(hidden, lax.dynamic_index_in_dim(w_exp_down, expert_index, 0, False), preferred_element_type=single)
        addend = jnp.where(live_rows[:, None], jnp.take(row_weight, picked)[:, None] * expert_out, 0.0)
        return (running.at[picked].add(addend), None)
    routed, _ = lax.scan(expert_step, jnp.zeros((SEQS, D), single), jnp.arange(EXPERTS, dtype=jnp.int32))
    contract = (((1,), (1,)), ((), ()))
    dense_gate_pre = lax.dot_general(normed2, w_dense_gate, contract, preferred_element_type=single)
    dense_up_pre = lax.dot_general(normed2, w_dense_up, contract, preferred_element_type=single)
    dense_hidden = (jax.nn.silu(dense_gate_pre) * dense_up_pre).astype(jnp.bfloat16)
    dense_out = jnp.dot(dense_hidden, w_dense_down, preferred_element_type=single)
    return (residual + routed + branch_weight[:, None] * dense_out).astype(jnp.bfloat16)
```

```python
import functools
import math

import jax
import jax.numpy as jnp
from jax import lax
from jax.experimental import pallas as pl
from jax.experimental.pallas import tpu as pltpu
from jax.sharding import PartitionSpec as P

HEADS = 16
HEAD = 64
KV_HEADS = 8

epsilon = 1e-06
MESH = pl.DeviceIdType.MESH
single = jnp.float32
half = jnp.bfloat16


def softplus(z):
    return jnp.maximum(z, 0.0) + jnp.log1p(jnp.exp(-jnp.abs(z)))


def mul(a, b):
    return jnp.dot(a, b, preferred_element_type=single)


def mul_rows(a, b):
    return lax.dot_general(a, b, (((1,), (1,)), ((), ())), preferred_element_type=single)


def gated(gate_pre, up_pre):
    return (gate_pre / (1.0 + jnp.exp(-gate_pre)) * up_pre).astype(half)


def remote(src, dst, send, recv, axis, peer):
    return pltpu.make_async_remote_copy(
        src_ref=src,
        dst_ref=dst,
        send_sem=send,
        recv_sem=recv,
        device_id={axis: peer},
        device_id_type=MESH,
    )


def layer_kernel(
    ep_n,
    tp_n,
    tokens,
    attn_gain,
    w_query,
    stick_bias,
    kv_cache,
    lengths,
    head_gain,
    w_attn_out,
    ffn_gain,
    route_expert,
    route_weight,
    w_exp_gate,
    w_exp_up,
    w_exp_down,
    branch_gate,
    w_dense_gate,
    w_dense_up,
    w_dense_down,
    out,
    wq,
    kv,
    wo,
    eg,
    eu,
    ed,
    dg,
    du,
    dd,
    grid,
    att,
    att_send,
    att_recv,
    rows_all,
    routes,
    x,
    hidden,
    pair_send,
    pair_recv,
    y_send,
    y_recv,
    own,
    ep_send,
    ep_recv,
    load_sem,
    kv_sem,
    exp_sem,
    att_sems,
    route_sems,
    gather_sems,
    mate_sems,
    far_sems,
    relay_sems,
    pair_sems,
    y_sems,
    ep_sems,
):
    me_ep, me_tp = lax.axis_index("ep"), lax.axis_index("tp")
    mate = me_tp + 1 - 2 * lax.rem(me_tp, 2)
    y_n = tp_n // 2
    seqs, width = tokens.shape
    part = width // tp_n
    rows = ep_n * seqs
    kv_n = kv_cache.shape[1]
    positions = kv_cache.shape[2]
    heads = kv_n * 2
    score_rows = seqs * heads
    experts = w_exp_gate.shape[0]
    tile_seqs = 8 // heads

    def ep_peer(d):
        return lax.rem(me_ep + d, ep_n)

    def tp_peer(d):
        return lax.rem(me_tp + d, tp_n)

    barrier = pltpu.get_barrier_semaphore()
    for d in range(1, ep_n):
        pl.semaphore_signal(barrier, inc=1, device_id={"ep": ep_peer(d)}, device_id_type=MESH)
    for d in range(1, tp_n):
        pl.semaphore_signal(barrier, inc=1, device_id={"tp": tp_peer(d)}, device_id_type=MESH)

    load_q = pltpu.make_async_copy(w_query, wq, load_sem.at[0])
    load_q.start()
    load_kv = []
    for s in range(seqs):
        load_kv.append(pltpu.make_async_copy(kv_cache.at[s], kv.at[s], kv_sem.at[s]))
        load_kv[-1].start()

    wide = tokens[...].astype(single)
    mean_sq = jnp.mean(wide * wide, axis=-1, keepdims=True)
    normed = (wide * lax.rsqrt(mean_sq + epsilon) * attn_gain[...]).astype(half)
    load_q.wait()
    query = mul(normed, wq[...]).astype(half)

    load_o = pltpu.make_async_copy(w_attn_out, wo, load_sem.at[1])
    load_o.start()
    load_d = []
    for i, (src, dst) in enumerate(((w_dense_gate, dg), (w_dense_up, du), (w_dense_down, dd))):
        load_d.append(pltpu.make_async_copy(src, dst, load_sem.at[2 + i]))
        load_d[-1].start()

    exp_pairs = ((w_exp_gate, eg), (w_exp_up, eu), (w_exp_down, ed))

    def exp_load(i, e):
        src, dst = exp_pairs[i]
        return pltpu.make_async_copy(src.at[e], dst.at[e], exp_sem.at[i, e])

    for e in range(experts):
        exp_load(0, e).start()
        exp_load(1, e).start()
    for e in range(experts):
        exp_load(2, e).start()

    spread = lax.broadcasted_iota(jnp.int32, (score_rows, seqs), 0) // heads
    spread = (spread == lax.broadcasted_iota(jnp.int32, (score_rows, seqs), 1)).astype(half)
    fold = lax.broadcasted_iota(jnp.int32, (seqs, score_rows), 1) // heads
    fold = (fold == lax.broadcasted_iota(jnp.int32, (seqs, score_rows), 0)).astype(half)
    row_id = lax.broadcasted_iota(jnp.int32, (score_rows, 128), 0)
    lane_id = lax.broadcasted_iota(jnp.int32, (score_rows, 128), 1)
    head_id = row_id % heads
    odd = head_id % 2 == 1
    query_rep = mul(spread, query)
    blocks = []
    for k in range(kv_n):
        piece = query_rep[:, k * 128 : (k + 1) * 128]
        piece = jnp.where(odd, pltpu.roll(piece, HEAD, 1), piece)
        keep = (lane_id < HEAD) & (head_id // 2 == k)
        blocks.append(jnp.where(keep, piece, 0.0) * (1.0 / math.sqrt(HEAD)))
    query_blk = jnp.concatenate(blocks, axis=1) if kv_n > 1 else blocks[0]

    def cache_of(s):
        return jnp.concatenate([kv[s, k] for k in range(kv_n)], axis=1) if kv_n > 1 else kv[s, 0]

    tile_row = lax.broadcasted_iota(jnp.int32, (8, 128), 0)[:, :1] // heads
    for p in range(score_rows // 8):
        total = None
        q_tile = query_blk[p * 8 : (p + 1) * 8]
        for u in range(tile_seqs):
            s = p * tile_seqs + u
            load_kv[s].wait()
            term = mul_rows(jnp.where(tile_row == u, q_tile, 0.0).astype(half), cache_of(s))
            total = term if total is None else total + term
        grid[p * 8 : (p + 1) * 8, :] = total

    row_col = row_id[:, :1]
    seq_col, head_col = row_col // heads, row_col % heads
    length_col = jnp.zeros_like(row_col)
    for s in range(seqs):
        length_col = jnp.where(seq_col == s, lengths[s], length_col)
    bias_col = jnp.zeros(row_col.shape, single)
    for h in range(heads):
        bias_col = jnp.where(head_col == h, stick_bias[h], bias_col)
    span = 256
    later = lax.broadcasted_iota(jnp.int32, (span, span), 0)
    later = (later >= lax.broadcasted_iota(jnp.int32, (span, span), 1)).astype(half)
    span_lane = lax.broadcasted_iota(jnp.int32, (score_rows, span), 1)
    carry = jnp.zeros(row_col.shape, single)
    for t in reversed(range(positions // span)):
        z = grid[:, t * span : (t + 1) * span] + bias_col
        valid = span_lane + t * span < length_col
        plus = jnp.where(valid, softplus(z), 0.0)
        high = plus.astype(half)
        rest = plus - high.astype(single)
        mid = rest.astype(half)
        low = (rest - mid.astype(single)).astype(half)
        suffix = mul(high, later) + (mul(mid, later) + mul(low, later)) + carry
        carry = suffix[:, :1]
        grid[:, t * span : (t + 1) * span] = jnp.where(valid, jnp.exp(z - suffix), 0.0)

    tiles = []
    for p in range(score_rows // 8):
        total = None
        w_tile = grid[p * 8 : (p + 1) * 8, :]
        for u in range(tile_seqs):
            s = p * tile_seqs + u
            term = mul(jnp.where(tile_row == u, w_tile, 0.0).astype(half), cache_of(s))
            total = term if total is None else total + term
        tiles.append(total)
    head_out = jnp.concatenate(tiles, axis=0)
    blocks = []
    for k in range(kv_n):
        piece = head_out[:, k * 128 : (k + 1) * 128]
        square = jnp.where(lane_id >= HEAD, piece * piece, 0.0)
        scale = lax.rsqrt(jnp.sum(square, axis=-1, keepdims=True) / HEAD + epsilon)
        piece = piece * scale
        piece = jnp.where(odd, piece, pltpu.roll(piece, HEAD, 1))
        piece = piece * head_gain[:, k * 128 : (k + 1) * 128]
        keep = (lane_id // HEAD == head_id % 2) & (head_id // 2 == k)
        blocks.append(jnp.where(keep, piece, 0.0))
    head_rows = jnp.concatenate(blocks, axis=1) if kv_n > 1 else blocks[0]
    head_rows = mul(fold, head_rows.astype(half)).astype(half)
    load_o.wait()
    for c in range(tp_n):
        piece = mul(head_rows, wo[:, c * part : (c + 1) * part])
        att[c] = piece
        att_send[c] = piece.astype(half)

    ids = route_expert[...].astype(single)
    weights = route_weight[...].astype(single)
    lane = lax.broadcasted_iota(jnp.int32, (seqs, 128), 1)
    packed = jnp.where(
        lane == 0,
        ids[:, 0:1],
        jnp.where(
            lane == 1,
            ids[:, 1:2],
            jnp.where(lane == 2, weights[:, 0:1], jnp.where(lane == 3, weights[:, 1:2], 0.0)),
        ),
    )
    routes[me_ep] = packed.astype(half)

    pl.semaphore_wait(barrier, ep_n + tp_n - 2)

    pending = []
    att_copies = []
    for d in range(1, tp_n):
        copy = remote(
            att_send.at[tp_peer(d)],
            att_recv.at[d],
            att_sems.at[0, d],
            att_sems.at[1, d],
            "tp",
            tp_peer(d),
        )
        copy.start()
        att_copies.append(copy)
    route_copies = []
    for d in range(1, ep_n):
        copy = remote(
            routes.at[me_ep],
            routes.at[me_ep],
            route_sems.at[0, d],
            route_sems.at[1, d],
            "ep",
            ep_peer(d),
        )
        copy.start()
        route_copies.append(copy)
    cols = pl.ds(pl.multiple_of(me_tp * part, part), part)
    residual = att[me_tp]
    for d in range(1, tp_n):
        att_copies[d - 1].wait_recv()
        residual = residual + att_recv[d].astype(single)
    residual = tokens[:, cols].astype(single) + residual
    rows_all[me_tp, me_ep] = residual.astype(half)
    pending += att_copies + route_copies

    gather_copies = [None]
    for d in range(1, ep_n):
        copy = remote(
            rows_all.at[me_tp, me_ep],
            rows_all.at[me_tp, me_ep],
            gather_sems.at[0, d],
            gather_sems.at[1, d],
            "ep",
            ep_peer(d),
        )
        copy.start()
        gather_copies.append(copy)
    pending += gather_copies[1:]
    mates, fars, relays = [], {}, []
    for d in range(ep_n):
        source = lax.rem(me_ep + ep_n - d, ep_n)
        if d:
            gather_copies[d].wait_recv()
        block = rows_all.at[me_tp, source]
        for y in range(1, y_n):
            copy = remote(
                block, block, far_sems.at[0, y, d], far_sems.at[1, y, d], "tp", tp_peer(2 * y)
            )
            copy.start()
            fars[y, d] = copy
        copy = remote(block, block, mate_sems.at[0, d], mate_sems.at[1, d], "tp", mate)
        copy.start()
        mates.append(copy)
    for d in range(ep_n):
        source = lax.rem(me_ep + ep_n - d, ep_n)
        for y in range(1, y_n):
            fars[y, d].wait_recv()
            block = rows_all.at[lax.rem(me_tp + tp_n - 2 * y, tp_n), source]
            copy = remote(
                block, block, relay_sems.at[0, y, d], relay_sems.at[1, y, d], "tp", mate
            )
            copy.start()
            relays.append(copy)
    for copy in route_copies + mates + relays:
        copy.wait_recv()
    pending += mates + list(fars.values()) + relays

    square = jnp.zeros((rows, 1), single)
    for c in range(tp_n):
        piece = rows_all[c].reshape(rows, part).astype(single)
        square = square + jnp.sum(piece * piece, axis=-1, keepdims=True)
    scale = lax.rsqrt(square / width + epsilon)
    logit = jnp.zeros((rows, 1), single)
    for c in range(tp_n):
        span_c = slice(c * part, (c + 1) * part)
        piece = rows_all[c].reshape(rows, part).astype(single)
        piece = (piece * scale * ffn_gain[:, span_c]).astype(half)
        x[:, span_c] = piece
        product = piece.astype(single) * branch_gate[:, span_c].astype(single)
        logit = logit + jnp.sum(product, axis=-1, keepdims=True)
    branch = (1.0 / (1.0 + jnp.exp(-logit))).astype(half).astype(single)
    route = routes[...].reshape(rows, 128).astype(single)

    def coefficient(e):
        own_id = (me_ep * experts + e).astype(single)
        first = jnp.where(route[:, 0:1] == own_id, route[:, 2:3], 0.0)
        return first + jnp.where(route[:, 1:2] == own_id, route[:, 3:4], 0.0)

    for load in load_d:
        load.wait()
    dense = gated(mul_rows(x[...], dg[...]), mul_rows(x[...], du[...]))

    def expert_step(e, carried):
        exp_load(0, e).wait()
        exp_load(1, e).wait()
        hidden[e] = gated(mul(x[...], eg[e]), mul(x[...], eu[e]))
        return carried

    lax.fori_loop(0, experts, expert_step, 0)
    for e in range(experts):
        exp_load(2, e).wait()
    coefs = [coefficient(e) for e in range(experts)]

    def chunk(target):
        at = pl.ds(pl.multiple_of(target * part, part), part)
        total = branch * mul(dense, dd[:, at])
        for e in range(experts):
            total = total + coefs[e] * mul(hidden[e], ed[e, :, at])
        return total

    pair_copies = []
    order = list(range(1, y_n)) + [0]
    for y in order:
        pair_send[y] = chunk(lax.rem(mate + 2 * y, tp_n)).astype(half)
        copy = remote(
            pair_send.at[y], pair_recv.at[y], pair_sems.at[0, y], pair_sems.at[1, y], "tp", mate
        )
        copy.start()
        pair_copies.append(copy)
    y_copies = {}
    for copy, y in zip(pair_copies, order):
        total = chunk(tp_peer(2 * y))
        copy.wait_recv()
        total = total + pair_recv[y].astype(single)
        if y == 0:
            own[...] = total.reshape(ep_n, seqs, part)
            continue
        y_send[y] = total.astype(half).reshape(ep_n, seqs, part)
        for d in list(range(1, ep_n)) + [0]:
            copy = remote(
                y_send.at[y, ep_peer(d)],
                y_recv.at[y, ep_peer(d)],
                y_sems.at[0, y, d],
                y_sems.at[1, y, d],
                "tp",
                tp_peer(2 * y),
            )
            copy.start()
            y_copies[y, d] = copy
    pending += pair_copies + list(y_copies.values())
    ep_copies = []
    for d in list(range(1, ep_n)) + [0]:
        target = ep_peer(d)
        total = own[target]
        for y in range(1, y_n):
            y_copies[y, d].wait_recv()
            total = total + y_recv[y, target].astype(single)
        if d == 0:
            residual = residual + total
            continue
        ep_send[d] = total.astype(half)
        copy = remote(
            ep_send.at[d], ep_recv.at[d], ep_sems.at[0, d], ep_sems.at[1, d], "ep", target
        )
        copy.start()
        ep_copies.append(copy)
    for d in range(1, ep_n):
        ep_copies[d - 1].wait_recv()
        residual = residual + ep_recv[d].astype(single)
    out[...] = residual.astype(half)
    for copy in pending + ep_copies:
        copy.wait_send()


def shards(
    tokens,
    attn_gain,
    w_query,
    stick_bias,
    kv_cache,
    lengths,
    head_gain,
    w_attn_out,
    ffn_gain,
    route_expert,
    route_weight,
    w_exp_gate,
    w_exp_up,
    w_exp_down,
    branch_gate,
    w_dense_gate,
    w_dense_up,
    w_dense_down,
):
    ep_n = lax.axis_size("ep")
    tp_n = lax.axis_size("tp")
    seqs, width = tokens.shape
    part = width // tp_n
    rows = ep_n * seqs
    y_n = tp_n // 2
    kv_n, positions = kv_cache.shape[1:3]
    experts = w_exp_gate.shape[0]
    score_rows = seqs * kv_n * (HEADS // KV_HEADS)
    vmem = pl.BlockSpec(memory_space=pltpu.VMEM)
    smem = pl.BlockSpec(memory_space=pltpu.SMEM)
    hbm = pl.BlockSpec(memory_space=pl.ANY)
    dma = pltpu.SemaphoreType.DMA

    def like(array):
        return pltpu.VMEM(array.shape, array.dtype)

    return pl.pallas_call(
        functools.partial(layer_kernel, ep_n, tp_n),
        out_shape=jax.ShapeDtypeStruct((seqs, part), half),
        in_specs=[
            vmem,
            vmem,
            hbm,
            smem,
            hbm,
            smem,
            vmem,
            hbm,
            vmem,
            vmem,
            vmem,
            hbm,
            hbm,
            hbm,
            vmem,
            hbm,
            hbm,
            hbm,
        ],
        out_specs=vmem,
        scratch_shapes=[
            like(w_query),
            like(kv_cache),
            like(w_attn_out),
            like(w_exp_gate),
            like(w_exp_up),
            like(w_exp_down),
            like(w_dense_gate),
            like(w_dense_up),
            like(w_dense_down),
            pltpu.VMEM((score_rows, positions), single),
            pltpu.VMEM((tp_n, seqs, part), single),
            pltpu.VMEM((tp_n, seqs, part), half),
            pltpu.VMEM((tp_n, seqs, part), half),
            pltpu.VMEM((tp_n, ep_n, seqs, part), half),
            pltpu.VMEM((ep_n, seqs, 128), half),
            pltpu.VMEM((rows, width), half),
            pltpu.VMEM((experts, rows, w_exp_gate.shape[2]), half),
            pltpu.VMEM((y_n, rows, part), half),
            pltpu.VMEM((y_n, rows, part), half),
            pltpu.VMEM((y_n, ep_n, seqs, part), half),
            pltpu.VMEM((y_n, ep_n, seqs, part), half),
            pltpu.VMEM((ep_n, seqs, part), single),
            pltpu.VMEM((ep_n, seqs, part), half),
            pltpu.VMEM((ep_n, seqs, part), half),
            dma((5,)),
            dma((seqs,)),
            dma((3, experts)),
            dma((2, tp_n)),
            dma((2, ep_n)),
            dma((2, ep_n)),
            dma((2, ep_n)),
            dma((2, y_n, ep_n)),
            dma((2, y_n, ep_n)),
            dma((2, y_n)),
            dma((2, y_n, ep_n)),
            dma((2, ep_n)),
        ],
        compiler_params=pltpu.CompilerParams(
            collective_id=0, has_side_effects=True, vmem_limit_bytes=60 * 1024 * 1024
        ),
    )(
        tokens,
        attn_gain.reshape(1, -1),
        w_query,
        stick_bias,
        kv_cache,
        lengths,
        head_gain.reshape(1, -1),
        w_attn_out,
        ffn_gain.reshape(1, -1),
        route_expert,
        route_weight,
        w_exp_gate,
        w_exp_up,
        w_exp_down,
        branch_gate.reshape(1, -1),
        w_dense_gate,
        w_dense_up,
        w_dense_down,
    )


def solution(mesh):
    return jax.shard_map(
        shards,
        mesh=mesh,
        in_specs=(
            P("ep", None),
            P(),
            P(None, "tp"),
            P("tp"),
            P("ep", "tp", None, None),
            P("ep"),
            P("tp"),
            P("tp", None),
            P(),
            P("ep", None),
            P("ep", None),
            P("ep", None, "tp"),
            P("ep", None, "tp"),
            P("ep", "tp", None),
            P(),
            P(("ep", "tp"), None),
            P(("ep", "tp"), None),
            P(("ep", "tp"), None),
        ),
        out_specs=P("ep", "tp"),
        check_vma=False,
    )
```

```python
import functools
import math

import jax
import jax.numpy as jnp
from jax import lax
from jax.experimental import pallas as pl
from jax.experimental.pallas import tpu as pltpu
from jax.sharding import PartitionSpec as P

HEADS = 16
HEAD = 64
KV_HEADS = 8

epsilon = 1e-06
MESH = pl.DeviceIdType.MESH
single = jnp.float32
half = jnp.bfloat16


def softplus(z):
    return jnp.maximum(z, 0.0) + jnp.log1p(jnp.exp(-jnp.abs(z)))


def mul(a, b):
    return jnp.dot(a, b, preferred_element_type=single)


def mul_rows(a, b):
    return lax.dot_general(a, b, (((1,), (1,)), ((), ())), preferred_element_type=single)


def gated(gate_pre, up_pre):
    return (gate_pre / (1.0 + jnp.exp(-gate_pre)) * up_pre).astype(half)


def remote(src, dst, send, recv, axis, peer):
    return pltpu.make_async_remote_copy(
        src_ref=src,
        dst_ref=dst,
        send_sem=send,
        recv_sem=recv,
        device_id={axis: peer},
        device_id_type=MESH,
    )


def layer_kernel(
    ep_n,
    tp_n,
    tokens,
    attn_gain,
    w_query,
    stick_bias,
    kv_cache,
    lengths,
    head_gain,
    w_attn_out,
    ffn_gain,
    route_expert,
    route_weight,
    w_exp_gate,
    w_exp_up,
    w_exp_down,
    branch_gate,
    w_dense_gate,
    w_dense_up,
    w_dense_down,
    out,
    wq,
    kv,
    wo,
    eg,
    eu,
    ed,
    dg,
    du,
    dd,
    grid,
    att,
    att_send,
    att_recv,
    rows_all,
    routes,
    x,
    hidden,
    pair_send,
    pair_recv,
    y_send,
    y_recv,
    own,
    ep_send,
    ep_recv,
    load_sem,
    kv_sem,
    exp_sem,
    att_sems,
    route_sems,
    gather_sems,
    mate_sems,
    far_sems,
    relay_sems,
    pair_sems,
    y_sems,
    ep_sems,
):
    me_ep, me_tp = lax.axis_index("ep"), lax.axis_index("tp")
    mate = me_tp + 1 - 2 * lax.rem(me_tp, 2)
    y_n = tp_n // 2
    seqs, width = tokens.shape
    part = width // tp_n
    rows = ep_n * seqs
    kv_n = kv_cache.shape[1]
    positions = kv_cache.shape[2]
    heads = kv_n * 2
    score_rows = seqs * heads
    experts = w_exp_gate.shape[0]
    tile_seqs = 8 // heads

    def ep_peer(d):
        return lax.rem(me_ep + d, ep_n)

    def tp_peer(d):
        return lax.rem(me_tp + d, tp_n)

    barrier = pltpu.get_barrier_semaphore()
    for d in range(1, ep_n):
        pl.semaphore_signal(barrier, inc=1, device_id={"ep": ep_peer(d)}, device_id_type=MESH)
    for d in range(1, tp_n):
        pl.semaphore_signal(barrier, inc=1, device_id={"tp": tp_peer(d)}, device_id_type=MESH)

    load_q = pltpu.make_async_copy(w_query, wq, load_sem.at[0])
    load_q.start()
    load_kv = []
    for s in range(seqs):
        load_kv.append(pltpu.make_async_copy(kv_cache.at[s], kv.at[s], kv_sem.at[s]))
        load_kv[-1].start()

    wide = tokens[...].astype(single)
    mean_sq = jnp.mean(wide * wide, axis=-1, keepdims=True)
    normed = (wide * lax.rsqrt(mean_sq + epsilon) * attn_gain[...]).astype(half)
    load_q.wait()
    query = mul(normed, wq[...]).astype(half)

    load_o = pltpu.make_async_copy(w_attn_out, wo, load_sem.at[1])
    load_o.start()
    load_d = []
    for i, (src, dst) in enumerate(((w_dense_gate, dg), (w_dense_up, du), (w_dense_down, dd))):
        load_d.append(pltpu.make_async_copy(src, dst, load_sem.at[2 + i]))
        load_d[-1].start()

    exp_pairs = ((w_exp_gate, eg), (w_exp_up, eu), (w_exp_down, ed))

    def exp_load(i, e):
        src, dst = exp_pairs[i]
        return pltpu.make_async_copy(src.at[e], dst.at[e], exp_sem.at[i, e])

    for e in range(experts):
        exp_load(0, e).start()
        exp_load(1, e).start()
    for e in range(experts):
        exp_load(2, e).start()

    spread = lax.broadcasted_iota(jnp.int32, (score_rows, seqs), 0) // heads
    spread = (spread == lax.broadcasted_iota(jnp.int32, (score_rows, seqs), 1)).astype(half)
    fold = lax.broadcasted_iota(jnp.int32, (seqs, score_rows), 1) // heads
    fold = (fold == lax.broadcasted_iota(jnp.int32, (seqs, score_rows), 0)).astype(half)
    row_id = lax.broadcasted_iota(jnp.int32, (score_rows, 128), 0)
    lane_id = lax.broadcasted_iota(jnp.int32, (score_rows, 128), 1)
    head_id = row_id % heads
    odd = head_id % 2 == 1
    query_rep = mul(spread, query)
    blocks = []
    for k in range(kv_n):
        piece = query_rep[:, k * 128 : (k + 1) * 128]
        piece = jnp.where(odd, pltpu.roll(piece, HEAD, 1), piece)
        keep = (lane_id < HEAD) & (head_id // 2 == k)
        blocks.append(jnp.where(keep, piece, 0.0) * (1.0 / math.sqrt(HEAD)))
    query_blk = jnp.concatenate(blocks, axis=1) if kv_n > 1 else blocks[0]

    def cache_of(s):
        return jnp.concatenate([kv[s, k] for k in range(kv_n)], axis=1) if kv_n > 1 else kv[s, 0]

    tile_row = lax.broadcasted_iota(jnp.int32, (8, 128), 0)[:, :1] // heads
    for p in range(score_rows // 8):
        total = None
        q_tile = query_blk[p * 8 : (p + 1) * 8]
        if p * tile_seqs % 4 == 0:
            for load in load_kv[p * tile_seqs : p * tile_seqs + 4]:
                load.wait()
        for u in range(tile_seqs):
            s = p * tile_seqs + u
            term = mul_rows(jnp.where(tile_row == u, q_tile, 0.0).astype(half), cache_of(s))
            total = term if total is None else total + term
        grid[p * 8 : (p + 1) * 8, :] = total

    row_col = row_id[:, :1]
    seq_col, head_col = row_col // heads, row_col % heads
    length_col = jnp.zeros_like(row_col)
    for s in range(seqs):
        length_col = jnp.where(seq_col == s, lengths[s], length_col)
    bias_col = jnp.zeros(row_col.shape, single)
    for h in range(heads):
        bias_col = jnp.where(head_col == h, stick_bias[h], bias_col)
    span = 256
    later = lax.broadcasted_iota(jnp.int32, (span, span), 0)
    later = (later >= lax.broadcasted_iota(jnp.int32, (span, span), 1)).astype(half)
    span_lane = lax.broadcasted_iota(jnp.int32, (score_rows, span), 1)
    carry = jnp.zeros(row_col.shape, single)
    for t in reversed(range(positions // span)):
        z = grid[:, t * span : (t + 1) * span] + bias_col
        valid = span_lane + t * span < length_col
        plus = jnp.where(valid, softplus(z), 0.0)
        high = plus.astype(half)
        rest = plus - high.astype(single)
        mid = rest.astype(half)
        low = (rest - mid.astype(single)).astype(half)
        suffix = mul(high, later) + (mul(mid, later) + mul(low, later)) + carry
        carry = suffix[:, :1]
        grid[:, t * span : (t + 1) * span] = jnp.where(valid, jnp.exp(z - suffix), 0.0)

    tiles = []
    for p in range(score_rows // 8):
        total = None
        w_tile = grid[p * 8 : (p + 1) * 8, :]
        for u in range(tile_seqs):
            s = p * tile_seqs + u
            term = mul(jnp.where(tile_row == u, w_tile, 0.0).astype(half), cache_of(s))
            total = term if total is None else total + term
        tiles.append(total)
    head_out = jnp.concatenate(tiles, axis=0)
    blocks = []
    for k in range(kv_n):
        piece = head_out[:, k * 128 : (k + 1) * 128]
        square = jnp.where(lane_id >= HEAD, piece * piece, 0.0)
        scale = lax.rsqrt(jnp.sum(square, axis=-1, keepdims=True) / HEAD + epsilon)
        piece = piece * scale
        piece = jnp.where(odd, piece, pltpu.roll(piece, HEAD, 1))
        piece = piece * head_gain[:, k * 128 : (k + 1) * 128]
        keep = (lane_id // HEAD == head_id % 2) & (head_id // 2 == k)
        blocks.append(jnp.where(keep, piece, 0.0))
    head_rows = jnp.concatenate(blocks, axis=1) if kv_n > 1 else blocks[0]
    head_rows = mul(fold, head_rows.astype(half)).astype(half)
    load_o.wait()
    for c in range(tp_n):
        piece = mul(head_rows, wo[:, c * part : (c + 1) * part])
        att[c] = piece
        att_send[c] = piece.astype(half)

    eye = lax.broadcasted_iota(jnp.int32, (seqs, seqs), 0)
    eye = eye == lax.broadcasted_iota(jnp.int32, (seqs, seqs), 1)

    def upright(row):
        return jnp.sum(jnp.where(eye, row.astype(single), 0.0), axis=1, keepdims=True)

    ids = [upright(route_expert[j : j + 1, :]) for j in range(2)]
    weights = [upright(route_weight[j : j + 1, :]) for j in range(2)]
    lane = lax.broadcasted_iota(jnp.int32, (seqs, 128), 1)
    packed = jnp.where(
        lane == 0,
        ids[0],
        jnp.where(
            lane == 1,
            ids[1],
            jnp.where(lane == 2, weights[0], jnp.where(lane == 3, weights[1], 0.0)),
        ),
    )
    routes[me_ep] = packed.astype(half)

    pl.semaphore_wait(barrier, ep_n + tp_n - 2)

    pending = []
    att_copies = []
    for d in range(1, tp_n):
        copy = remote(
            att_send.at[tp_peer(d)],
            att_recv.at[d],
            att_sems.at[0, d],
            att_sems.at[1, d],
            "tp",
            tp_peer(d),
        )
        copy.start()
        att_copies.append(copy)
    route_copies = []
    for d in range(1, ep_n):
        copy = remote(
            routes.at[me_ep],
            routes.at[me_ep],
            route_sems.at[0, d],
            route_sems.at[1, d],
            "ep",
            ep_peer(d),
        )
        copy.start()
        route_copies.append(copy)
    cols = pl.ds(pl.multiple_of(me_tp * part, part), part)
    residual = att[me_tp]
    for d in range(1, tp_n):
        att_copies[d - 1].wait_recv()
        residual = residual + att_recv[d].astype(single)
    residual = tokens[:, cols].astype(single) + residual
    rows_all[me_tp, me_ep] = residual.astype(half)
    pending += att_copies + route_copies

    gather_copies = [None]
    for d in range(1, ep_n):
        copy = remote(
            rows_all.at[me_tp, me_ep],
            rows_all.at[me_tp, me_ep],
            gather_sems.at[0, d],
            gather_sems.at[1, d],
            "ep",
            ep_peer(d),
        )
        copy.start()
        gather_copies.append(copy)
    pending += gather_copies[1:]
    mates, fars, relays = [], {}, []
    for d in range(ep_n):
        source = lax.rem(me_ep + ep_n - d, ep_n)
        if d:
            gather_copies[d].wait_recv()
        block = rows_all.at[me_tp, source]
        for y in range(1, y_n):
            copy = remote(
                block, block, far_sems.at[0, y, d], far_sems.at[1, y, d], "tp", tp_peer(2 * y)
            )
            copy.start()
            fars[y, d] = copy
        copy = remote(block, block, mate_sems.at[0, d], mate_sems.at[1, d], "tp", mate)
        copy.start()
        mates.append(copy)
    for d in range(ep_n):
        source = lax.rem(me_ep + ep_n - d, ep_n)
        for y in range(1, y_n):
            fars[y, d].wait_recv()
            block = rows_all.at[lax.rem(me_tp + tp_n - 2 * y, tp_n), source]
            copy = remote(
                block, block, relay_sems.at[0, y, d], relay_sems.at[1, y, d], "tp", mate
            )
            copy.start()
            relays.append(copy)
    for copy in route_copies + mates + relays:
        copy.wait_recv()
    pending += mates + list(fars.values()) + relays

    square = jnp.zeros((rows, 1), single)
    for c in range(tp_n):
        piece = rows_all[c].reshape(rows, part).astype(single)
        square = square + jnp.sum(piece * piece, axis=-1, keepdims=True)
    scale = lax.rsqrt(square / width + epsilon)
    logit = jnp.zeros((rows, 1), single)
    branch_row = branch_gate[...].astype(single).reshape(1, width)
    for c in range(tp_n):
        span_c = slice(c * part, (c + 1) * part)
        piece = rows_all[c].reshape(rows, part).astype(single)
        piece = (piece * scale * ffn_gain[:, span_c]).astype(half)
        x[:, span_c] = piece
        product = piece.astype(single) * branch_row[:, span_c]
        logit = logit + jnp.sum(product, axis=-1, keepdims=True)
    branch = (1.0 / (1.0 + jnp.exp(-logit))).astype(half).astype(single)
    route = routes[...].reshape(rows, 128).astype(single)

    def coefficient(e):
        own_id = (me_ep * experts + e).astype(single)
        first = jnp.where(route[:, 0:1] == own_id, route[:, 2:3], 0.0)
        return first + jnp.where(route[:, 1:2] == own_id, route[:, 3:4], 0.0)

    for load in load_d:
        load.wait()
    dense = gated(mul_rows(x[...], dg[...]), mul_rows(x[...], du[...]))

    def expert_step(e, carried):
        exp_load(0, e).wait()
        exp_load(1, e).wait()
        hidden[e] = gated(mul(x[...], eg[e]), mul(x[...], eu[e]))
        return carried

    lax.fori_loop(0, experts, expert_step, 0)
    for e in range(experts):
        exp_load(2, e).wait()
    coefs = [coefficient(e) for e in range(experts)]

    def chunk(target):
        at = pl.ds(pl.multiple_of(target * part, part), part)
        total = branch * mul(dense, dd[:, at])
        for e in range(experts):
            total = total + coefs[e] * mul(hidden[e], ed[e, :, at])
        return total

    pair_copies = []
    order = list(range(1, y_n)) + [0]
    for y in order:
        pair_send[y] = chunk(lax.rem(mate + 2 * y, tp_n)).astype(half)
        copy = remote(
            pair_send.at[y], pair_recv.at[y], pair_sems.at[0, y], pair_sems.at[1, y], "tp", mate
        )
        copy.start()
        pair_copies.append(copy)
    y_copies = {}
    for copy, y in zip(pair_copies, order):
        total = chunk(tp_peer(2 * y))
        copy.wait_recv()
        total = total + pair_recv[y].astype(single)
        if y == 0:
            own[...] = total.reshape(ep_n, seqs, part)
            continue
        y_send[y] = total.astype(half).reshape(ep_n, seqs, part)
        for d in list(range(1, ep_n)) + [0]:
            copy = remote(
                y_send.at[y, ep_peer(d)],
                y_recv.at[y, ep_peer(d)],
                y_sems.at[0, y, d],
                y_sems.at[1, y, d],
                "tp",
                tp_peer(2 * y),
            )
            copy.start()
            y_copies[y, d] = copy
    pending += pair_copies + list(y_copies.values())
    ep_copies = []
    for d in list(range(1, ep_n)) + [0]:
        target = ep_peer(d)
        total = own[target]
        for y in range(1, y_n):
            y_copies[y, d].wait_recv()
            total = total + y_recv[y, target].astype(single)
        if d == 0:
            residual = residual + total
            continue
        ep_send[d] = total.astype(half)
        copy = remote(
            ep_send.at[d], ep_recv.at[d], ep_sems.at[0, d], ep_sems.at[1, d], "ep", target
        )
        copy.start()
        ep_copies.append(copy)
    for d in range(1, ep_n):
        ep_copies[d - 1].wait_recv()
        residual = residual + ep_recv[d].astype(single)
    out[...] = residual.astype(half)
    for copy in pending + ep_copies:
        copy.wait_send()


def shards(
    tokens,
    attn_gain,
    w_query,
    stick_bias,
    kv_cache,
    lengths,
    head_gain,
    w_attn_out,
    ffn_gain,
    route_expert,
    route_weight,
    w_exp_gate,
    w_exp_up,
    w_exp_down,
    branch_gate,
    w_dense_gate,
    w_dense_up,
    w_dense_down,
):
    ep_n = lax.axis_size("ep")
    tp_n = lax.axis_size("tp")
    seqs, width = tokens.shape
    part = width // tp_n
    rows = ep_n * seqs
    y_n = tp_n // 2
    kv_n, positions = kv_cache.shape[1:3]
    experts = w_exp_gate.shape[0]
    score_rows = seqs * kv_n * (HEADS // KV_HEADS)
    vmem = pl.BlockSpec(memory_space=pltpu.VMEM)
    smem = pl.BlockSpec(memory_space=pltpu.SMEM)
    hbm = pl.BlockSpec(memory_space=pl.ANY)
    dma = pltpu.SemaphoreType.DMA

    def like(array):
        return pltpu.VMEM(array.shape, array.dtype)

    return pl.pallas_call(
        functools.partial(layer_kernel, ep_n, tp_n),
        out_shape=jax.ShapeDtypeStruct((seqs, part), half),
        in_specs=[
            vmem,
            vmem,
            hbm,
            smem,
            hbm,
            smem,
            vmem,
            hbm,
            vmem,
            vmem,
            vmem,
            hbm,
            hbm,
            hbm,
            vmem,
            hbm,
            hbm,
            hbm,
        ],
        out_specs=vmem,
        scratch_shapes=[
            like(w_query),
            like(kv_cache),
            like(w_attn_out),
            like(w_exp_gate),
            like(w_exp_up),
            like(w_exp_down),
            like(w_dense_gate),
            like(w_dense_up),
            like(w_dense_down),
            pltpu.VMEM((score_rows, positions), single),
            pltpu.VMEM((tp_n, seqs, part), single),
            pltpu.VMEM((tp_n, seqs, part), half),
            pltpu.VMEM((tp_n, seqs, part), half),
            pltpu.VMEM((tp_n, ep_n, seqs, part), half),
            pltpu.VMEM((ep_n, seqs, 128), half),
            pltpu.VMEM((rows, width), half),
            pltpu.VMEM((experts, rows, w_exp_gate.shape[2]), half),
            pltpu.VMEM((y_n, rows, part), half),
            pltpu.VMEM((y_n, rows, part), half),
            pltpu.VMEM((y_n, ep_n, seqs, part), half),
            pltpu.VMEM((y_n, ep_n, seqs, part), half),
            pltpu.VMEM((ep_n, seqs, part), single),
            pltpu.VMEM((ep_n, seqs, part), half),
            pltpu.VMEM((ep_n, seqs, part), half),
            dma((5,)),
            dma((seqs,)),
            dma((3, experts)),
            dma((2, tp_n)),
            dma((2, ep_n)),
            dma((2, ep_n)),
            dma((2, ep_n)),
            dma((2, y_n, ep_n)),
            dma((2, y_n, ep_n)),
            dma((2, y_n)),
            dma((2, y_n, ep_n)),
            dma((2, ep_n)),
        ],
        compiler_params=pltpu.CompilerParams(
            collective_id=0, has_side_effects=True, vmem_limit_bytes=60 * 1024 * 1024
        ),
    )(
        tokens,
        attn_gain.reshape(1, -1),
        w_query,
        stick_bias,
        kv_cache,
        lengths,
        head_gain.reshape(1, -1),
        w_attn_out,
        ffn_gain.reshape(1, -1),
        route_expert.T,
        route_weight.T,
        w_exp_gate,
        w_exp_up,
        w_exp_down,
        branch_gate,
        w_dense_gate,
        w_dense_up,
        w_dense_down,
    )


def solution(mesh):
    return jax.shard_map(
        shards,
        mesh=mesh,
        in_specs=(
            P("ep", None),
            P(),
            P(None, "tp"),
            P("tp"),
            P("ep", "tp", None, None),
            P("ep"),
            P("tp"),
            P("tp", None),
            P(),
            P("ep", None),
            P("ep", None),
            P("ep", None, "tp"),
            P("ep", None, "tp"),
            P("ep", "tp", None),
            P(),
            P(("ep", "tp"), None),
            P(("ep", "tp"), None),
            P(("ep", "tp"), None),
        ),
        out_specs=P("ep", "tp"),
        check_vma=False,
    )
```
